32 devices in a mesh: ep: 8 (over z, core), tp: 4 (over y, x).
Axes of the slice: x: 2, y: 2, z: 4, core: 2. Of those that a mesh axis runs over, the one named last changes fastest.
Arguments:
- tokens: bfloat16 [128, 2048], P('ep'), may hold values from -6 to 6
- old_state: float32 [128, 16, 128, 128], P('ep', 'tp'), may hold values from -2 to 2
- lower_bound: float32 [2048], P('tp'), may hold values from 0.05 to 0.95
- head_gain: float32 [2048], P('tp'), may hold values from 0.1 to 1.9
- norm_gains: float32 [4, 2048], replicated, may hold values from 0.1 to 1.9
- w_query: bfloat16 [2048, 2048], P('ep', 'tp'), may hold values from -0.125 to 0.125
- w_forget: bfloat16 [2048, 2048], P('ep', 'tp'), may hold values from -0.125 to 0.125
- w_value: bfloat16 [2048, 2048], P('ep', 'tp'), may hold values from -0.125 to 0.125
- w_outgate: bfloat16 [2048, 2048], P('ep', 'tp'), may hold values from -0.125 to 0.125
- w_mix_out: bfloat16 [2048, 2048], P('tp', 'ep'), may hold values from -0.125 to 0.125
- routes: int32 [128, 2], P('ep'), may hold values from 0 to 7, all different within a row; in each aligned block of 16 rows (0 to 15, 16 to 31, ...) at most 8 rows name the same one
- route_scores: float32 [128, 2], P('ep'), may hold values from -6 to 6
- w_exp_gate: bfloat16 [8, 2048, 3584], P('ep', None, 'tp'), may hold values from -0.125 to 0.125
- w_exp_up: bfloat16 [8, 2048, 3584], P('ep', None, 'tp'), may hold values from -0.125 to 0.125
- w_exp_down: bfloat16 [8, 3584, 2048], P('ep', 'tp'), may hold values from -0.75 to 0.75
- w_dense_gate: bfloat16 [2048, 6144], P('ep', 'tp'), may hold values from -0.125 to 0.125
- w_dense_up: bfloat16 [2048, 6144], P('ep', 'tp'), may hold values from -0.125 to 0.125
- w_dense_down: bfloat16 [6144, 2048], P('tp', 'ep'), may hold values from -0.75 to 0.75
- dense_mix: bfloat16 [2048], replicated, may hold values from -0.125 to 0.125
Outputs:
- layer_out: bfloat16 [128, 2048], P('ep', 'tp')
- new_state: float32 [128, 16, 128, 128], P('ep', 'tp')
The draws below stay inside these ranges and needn't reach their ends.
Inputs may be any that keep to these rules, and one draw needn't show every extreme that they name: `routes`: each row names 2 different experts. In each aligned block of 16 rows no expert is named by more than 8 rows, and in every draw some expert is named by exactly 8 rows of some block.
All inputs are finite; a program needn't handle non-finite values.
Results may differ from the reference program's by a relative error of at most 0.025.
Values may be sent and summed in bfloat16 or wider, within the bound.
No kernel may reach another device: no remote copies, remote signals or barrier semaphores. Data moves between devices by JAX's collectives and lax.ppermute only.
A program may use at most 64 MiB of HBM per device.

```python
import math
import jax
import jax.numpy as jnp
import numpy as np
from jax import lax

D = 2048
HEADS = 16
HEAD = 128
EXP_FF = 3584
DENSE_FF = 6144
TOPK = 2
SEQ_DEV = 16
HW = 2048
EXPERTS = 8
CAP = 8
TOKENS = 128
N_EP = 8
N_TP = 4


def column_scaled(key, leading, fan_in):
    noise_key = jax.random.fold_in(key, 11)
    spread_key = jax.random.fold_in(key, 23)
    position = jnp.arange(D, dtype=jnp.float32) / D
    base = jnp.clip(jax.random.normal(noise_key, leading + (D,), jnp.float32), -6.0, 6.0)
    profile = 10.0 ** position
    rough = jnp.exp(jax.random.uniform(spread_key, (D,), jnp.float32, -0.7, 0.7))
    return jnp.clip(base * profile * rough * fan_in ** (-0.5) / 3.0, -0.75, 0.75)


def draw_w_exp_down(key, part):
    return column_scaled(key, (EXPERTS, EXP_FF), EXP_FF).astype(jnp.bfloat16)


def draw_w_dense_down(key, part):
    return column_scaled(key, (DENSE_FF,), DENSE_FF).astype(jnp.bfloat16)


def level_of(key, shape, split, low, largest):
    gain, own = 1.0, jax.random.fold_in(key, 6)
    for axis_at, shards_of in split:
        steps = jnp.exp(jax.random.uniform(jax.random.fold_in(own, axis_at), (shards_of,), jnp.float32, low / len(split), largest / len(split)))
        gain = gain * jnp.repeat(steps, shape[axis_at] // shards_of).reshape([-1 if axis == axis_at else 1 for axis in range(len(shape))])
    return gain


def assign_block(own_key, own, number, rows, amount, top, reach, skew):
    sequence = jax.random.permutation(own_key, amount)
    crowded, ordinary = shares(amount, rows * top, reach, skew, True), shares(amount, rows * top, reach, skew, False)
    places = jnp.arange(amount)

    def named(tallies, rotation):
        used = int((tallies > 0).sum())
        fixed = max(1, used // 4)
        passed = fixed + (places - fixed + rotation * (used - fixed)) % max(1, amount - fixed)
        return jnp.zeros((amount,), jnp.int32).at[sequence[jnp.where(places < fixed, places, passed)]].set(jnp.asarray(tallies, jnp.int32))

    tallies = jnp.where(number % 4 == 0, named(crowded, number // 4), named(ordinary, number - number // 4 - 1))
    mixed = jax.random.permutation(jax.random.fold_in(own, 3), amount)
    donor, sink = mixed[0:amount // 2 * 2:2], mixed[1:amount // 2 * 2:2]
    margin = jnp.minimum(tallies[donor] - 1, reach - tallies[sink]) // 2
    margin = jnp.where((donor == sequence[0]) | (sink == sequence[0]) | (tallies[sink] == 0), 0, jnp.maximum(margin, 0))
    passed = jax.random.randint(jax.random.fold_in(own, 4), (amount // 2,), 0, 1 << 20) % (margin + 1)
    tallies = tallies.at[donor].add(-passed).at[sink].add(passed)
    items = jnp.searchsorted(jnp.cumsum(tallies), jnp.arange(rows * top), side="right").astype(jnp.int32)
    table = items.reshape(top, rows).T
    table = table[jax.random.permutation(jax.random.fold_in(own, 1), rows)]
    rotation = jax.random.randint(jax.random.fold_in(own, 2), (rows, 1), 0, top)
    return jnp.take_along_axis(table, (jnp.arange(top)[None, :] + rotation) % top, axis=1)


def shares(number_of, total, bound, skew, full):
    weights = [(1 << 20) // math.isqrt(grade ** skew) + 1 for grade in range(1, number_of + 1)]
    largest = bound if full else min(bound, max(-(-total // number_of), total * weights[0] // sum(weights)))
    least = 1 if total - largest >= number_of - 1 else 0
    holding, rest = [largest] + [least] * (number_of - 1), total - largest - least * (number_of - 1)
    while rest > 0:
        candidates = [i for i in range(1, number_of) if holding[i] < largest] or [i for i in range(1, number_of) if holding[i] < bound]
        mass, budget = sum([weights[i] for i in candidates]), rest
        for i in candidates:
            addition = min(bound - holding[i], max(1, budget * weights[i] // mass), rest)
            holding[i] = holding[i] + addition
            rest = rest - addition
    return np.array(holding)


def noise(key, shape, width, most, cuts=(), held_as=jnp.bfloat16):
    level = level_of(key, shape, cuts, -0.22, 0.18) if cuts else 1.0
    drawn = jax.random.normal(key, shape, jnp.float32) * width * level
    return jnp.minimum(jnp.maximum(drawn, -most), most).astype(held_as)


def setup_inputs(seed: int = 0) -> dict:
    keys = jax.random.split(jax.random.key(seed), 20)
    tokens = noise(keys[0], (TOKENS, D), 1.0, 6.0, ((0, 8),))
    old_state = noise(keys[1], (TOKENS, HEADS, HEAD, HEAD), 0.3, 2.0, ((0, 8), (1, 4)), jnp.float32)
    lower_bound = jnp.clip(0.05 + 0.9 * jax.random.uniform(keys[2], (HW,), jnp.float32) ** level_of(keys[2], (HW,), ((0, 4),), -0.2, 0.2), 0.05, 0.95)
    head_gain = jnp.clip(1.0 + 0.18 * jax.random.normal(keys[3], (HW,), jnp.float32), 0.1, 1.9)
    norm_gains = jnp.clip(1.0 + 0.18 * jax.random.normal(keys[4], (4, D), jnp.float32), 0.1, 1.9)
    w_query = noise(keys[5], (D, HW), D ** -0.5, 0.125, ((0, 8), (1, 4)))
    w_forget = noise(keys[6], (D, HW), D ** -0.5, 0.125, ((0, 8), (1, 4)))
    w_value = noise(keys[7], (D, HW), D ** -0.5, 0.125, ((0, 8), (1, 4)))
    w_outgate = noise(keys[8], (D, HW), D ** -0.5, 0.125, ((0, 8), (1, 4)))
    w_mix_out = noise(keys[9], (HW, D), HW ** -0.5, 0.125, ((0, 4), (1, 8)))
    routes_keys = jax.random.split(jax.random.fold_in(keys[10], 1), TOKENS // SEQ_DEV)
    routes_turns = jax.random.permutation(jax.random.fold_in(keys[10], 3), TOKENS // SEQ_DEV)
    routes = jax.vmap(lambda own, number: assign_block(jax.random.fold_in(keys[10], 2), own, number, SEQ_DEV, EXPERTS, TOPK, CAP, 1))(routes_keys, routes_turns).reshape((TOKENS, TOPK))
    route_scores = noise(keys[11], (TOKENS, TOPK), 1.5, 6.0, ((0, 8),), jnp.float32)
    w_exp_gate = noise(keys[12], (EXPERTS, D, EXP_FF), D ** -0.5, 0.125, ((0, 8), (2, 4)))
    w_exp_up = noise(keys[13], (EXPERTS, D, EXP_FF), D ** -0.5, 0.125, ((0, 8), (2, 4)))
    w_exp_down = draw_w_exp_down(jax.random.fold_in(keys[19], 71), 0)
    w_dense_gate = noise(keys[15], (D, DENSE_FF), D ** -0.5, 0.125, ((0, 8), (1, 4)))
    w_dense_up = noise(keys[16], (D, DENSE_FF), D ** -0.5, 0.125, ((0, 8), (1, 4)))
    w_dense_down = draw_w_dense_down(jax.random.fold_in(keys[19], 71), 0)
    dense_mix = noise(keys[18], (D,), D ** -0.5, 0.125)
    return dict(tokens=tokens, old_state=old_state, lower_bound=lower_bound, head_gain=head_gain, norm_gains=norm_gains, w_query=w_query, w_forget=w_forget, w_value=w_value, w_outgate=w_outgate, w_mix_out=w_mix_out, routes=routes, route_scores=route_scores, w_exp_gate=w_exp_gate, w_exp_up=w_exp_up, w_exp_down=w_exp_down, w_dense_gate=w_dense_gate, w_dense_up=w_dense_up, w_dense_down=w_dense_down, dense_mix=dense_mix)


EPS = 1e-06

def rms_scale(values):
    return lax.rsqrt(lax.optimization_barrier(jnp.mean(values * values, axis=-1, keepdims=True)) + EPS)

def reference(tokens, old_state, lower_bound, head_gain, norm_gains, w_query, w_forget, w_value, w_outgate, w_mix_out, routes, route_scores, w_exp_gate, w_exp_up, w_exp_down, w_dense_gate, w_dense_up, w_dense_down, dense_mix):
    highest = lax.Precision.HIGHEST
    resid = tokens.astype(jnp.float32)
    normed = (resid * rms_scale(resid) * norm_gains[0]).astype(jnp.bfloat16)
    query_raw = jnp.dot(normed, w_query, preferred_element_type=jnp.float32)
    forget_raw = jnp.dot(normed, w_forget, preferred_element_type=jnp.float32)
    value = jnp.dot(normed, w_value, preferred_element_type=jnp.float32)
    out_gate = jnp.dot(normed, w_outgate, preferred_element_type=jnp.float32)
    forget = lower_bound + (1.0 - lower_bound) * jax.nn.sigmoid(forget_raw)
    key_in = (1.0 - lower_bound) * jax.nn.sigmoid(-forget_raw)
    shape_heads = (TOKENS, HEADS, HEAD)
    new_state = forget.reshape(shape_heads)[..., None] * old_state + key_in.reshape(shape_heads)[..., None] * value.reshape(TOKENS, HEADS, 1, HEAD)
    query = jax.nn.silu(query_raw).reshape(shape_heads)
    read = jnp.einsum('thk,thkv->thv', query, new_state, precision=highest)
    gated = read * rms_scale(read) * head_gain.reshape(HEADS, HEAD) * jax.nn.silu(out_gate).reshape(shape_heads)
    mixed_heads = gated.reshape(TOKENS, HW).astype(jnp.bfloat16)
    groups = mixed_heads.reshape(TOKENS, N_TP, HW // N_TP).astype(jnp.float32)
    out_rows = w_mix_out.reshape(N_TP, HW // N_TP, D).astype(jnp.float32)
    mix_parts = jnp.einsum('tgk,gkd->gtd', groups, out_rows, precision=highest).astype(jnp.bfloat16)
    mix_out = lax.optimization_barrier(jnp.sum(mix_parts.astype(jnp.float32), axis=0)).astype(jnp.bfloat16)
    mix_wide = lax.optimization_barrier(mix_out).astype(jnp.float32)
    after_mix = resid + mix_wide * rms_scale(mix_wide) * norm_gains[1]
    ffn_in = (after_mix * rms_scale(after_mix) * norm_gains[2]).astype(jnp.bfloat16)
    blocks = routes.reshape(N_EP, SEQ_DEV * TOPK)
    expert_ids = jnp.arange(EXPERTS).astype(jnp.int32)
    onehot = (blocks[:, :, None] == expert_ids[None, None, :]).astype(jnp.int32)
    before = jnp.cumsum(onehot, axis=1).astype(jnp.int32) - onehot
    slots = lax.optimization_barrier(jnp.sum(onehot * before, axis=2)).astype(jnp.int32)
    route_rows = jnp.repeat(ffn_in.reshape(N_EP, SEQ_DEV, D), TOPK, axis=1).astype(jnp.float32)
    slot_ids = jnp.arange(CAP).astype(jnp.int32)

    def one_expert(index):
        chosen = ((blocks == index)[:, None, :] & (slots[:, None, :] == slot_ids[None, :, None])).astype(jnp.float32)
        expert_in = jnp.einsum('bcr,brd->bcd', chosen, route_rows, precision=highest).astype(jnp.bfloat16)
        expert_in = expert_in.reshape(N_EP * CAP, D)
        gate_pre = jnp.dot(expert_in, w_exp_gate[index], preferred_element_type=jnp.float32)
        up_pre = jnp.dot(expert_in, w_exp_up[index], preferred_element_type=jnp.float32)
        hidden = (jax.nn.silu(gate_pre) * up_pre).astype(jnp.bfloat16)
        hidden_groups = hidden.reshape(N_EP * CAP, N_TP, EXP_FF // N_TP).astype(jnp.float32)
        down_groups = w_exp_down[index].reshape(N_TP, EXP_FF // N_TP, D).astype(jnp.float32)
        parts = jnp.einsum('rgk,gkd->grd', hidden_groups, down_groups, precision=highest).astype(jnp.bfloat16)
        result = lax.optimization_barrier(jnp.sum(parts.astype(jnp.float32), axis=0)).astype(jnp.bfloat16)
        return result.reshape(N_EP, CAP, D)
    expert_out = lax.map(one_expert, expert_ids)
    block_ids = jnp.broadcast_to(jnp.arange(N_EP).astype(jnp.int32)[:, None], blocks.shape)
    picked = expert_out[blocks, block_ids, slots].astype(jnp.float32)
    first = jax.nn.sigmoid(route_scores[:, 0] - route_scores[:, 1])
    second = jax.nn.sigmoid(route_scores[:, 1] - route_scores[:, 0])
    route_weight = jnp.stack([first, second], axis=1).reshape(N_EP, SEQ_DEV * TOPK)
    weighted = (picked * route_weight[..., None]).reshape(N_EP, SEQ_DEV, TOPK, D)
    expert_sum = lax.optimization_barrier(jnp.sum(weighted, axis=2)).reshape(TOKENS, D)
    dense_gate_pre = jnp.dot(ffn_in, w_dense_gate, preferred_element_type=jnp.float32)
    dense_up_pre = jnp.dot(ffn_in, w_dense_up, preferred_element_type=jnp.float32)
    dense_hidden = (jax.nn.silu(dense_gate_pre) * dense_up_pre).astype(jnp.bfloat16)
    dense_out = jnp.dot(dense_hidden, w_dense_down, preferred_element_type=jnp.float32)
    mix_weight = jax.nn.sigmoid(jnp.dot(ffn_in, dense_mix, preferred_element_type=jnp.float32))
    ffn_out = expert_sum + mix_weight[:, None] * dense_out
    layer_out = (after_mix + ffn_out * rms_scale(ffn_out) * norm_gains[3]).astype(jnp.bfloat16)
    return (layer_out, new_state)
```

```python
import jax
import jax.numpy as jnp
from jax import lax
from jax.sharding import PartitionSpec as P

EPS = 1e-06
F32 = jnp.float32
BF16 = jnp.bfloat16


def rms_scale(values):
    return lax.rsqrt(jnp.mean(values * values, axis=-1, keepdims=True) + EPS)


def swap(value, axis, step):
    size = lax.axis_size(axis)
    return lax.ppermute(value, axis, [(i, i ^ step) for i in range(size)])


def relative_exchange(blocks):
    count = len(blocks)
    outward = jnp.stack(blocks[1::2])
    crossed = swap(outward, "ep", 1)
    pairs = [jnp.stack([blocks[2 * s], crossed[s]]) for s in range(count // 2)]
    arrived = [pairs[0]] + [swap(pairs[s], "ep", 2 * s) for s in range(1, count // 2)]
    return jnp.stack(arrived)


def relative_gather(block):
    half = lax.axis_size("ep") // 2
    even = [block] + [swap(block, "ep", 2 * s) for s in range(1, half)]
    odd = [swap(item, "ep", 1) for item in even]
    return jnp.stack([item for pair in zip(even, odd) for item in pair])


def relative_scatter_sum(partial):
    count, rows, width = partial.shape
    halves = partial.reshape(count // 2, 2, rows, width)
    crossed = swap(halves[:, 1].astype(BF16), "ep", 1)
    chip = halves[:, 0] + crossed.astype(F32)
    sent = chip[1:].astype(BF16)
    total = chip[0]
    for s in range(1, count // 2):
        total = total + swap(sent[s - 1], "ep", 2 * s).astype(F32)
    return total


def sum_over_tp(partial):
    sent = partial.astype(BF16)
    total = sent.astype(F32)
    for s in range(1, lax.axis_size("tp")):
        total = total + swap(sent, "tp", s).astype(F32)
    return total


def far_first_gather(block):
    stack = block[None]
    step = lax.axis_size("ep") // 2
    while step:
        stack = jnp.stack([stack, swap(stack, "ep", step)], axis=1).reshape((-1,) + block.shape)
        step //= 2
    return stack


def relative_to_absolute(values, index):
    rows, count, width = values.shape
    step = 1
    while step < count:
        split = values.reshape(rows, count // (2 * step), 2, step, width)
        values = jnp.where((index & step) != 0, split[:, :, ::-1], split).reshape(rows, count, width)
        step *= 2
    return values


def body(
    tokens,
    old_state,
    lower_bound,
    head_gain,
    norm_gains,
    w_query,
    w_forget,
    w_value,
    w_outgate,
    w_mix_out,
    routes,
    route_scores,
    w_exp_gate,
    w_exp_up,
    w_exp_down,
    w_dense_gate,
    w_dense_up,
    w_dense_down,
    dense_mix,
):
    seqs, width = tokens.shape
    ep_index = lax.axis_index("ep")
    ep_size = lax.axis_size("ep")
    column_index = lax.axis_index("tp")
    part_width = width // lax.axis_size("tp")
    feats = width // ep_size
    heads = old_state.shape[1]
    head_size = old_state.shape[2]
    local = heads * head_size

    mix_weights = far_first_gather(w_mix_out)

    resid = tokens.astype(F32)
    normed = (resid * rms_scale(resid) * norm_gains[0]).astype(BF16)
    mix_rows = relative_exchange(
        [
            lax.dynamic_slice_in_dim(normed, (ep_index ^ j) * feats, feats, 1)
            for j in range(ep_size)
        ]
    ).reshape(ep_size * seqs, feats)
    projected = jnp.concatenate(
        [
            jnp.dot(mix_rows, w, preferred_element_type=F32)
            for w in (w_query, w_forget, w_value, w_outgate)
        ],
        axis=1,
    ).reshape(ep_size, seqs, 4 * local)
    query_raw, forget_raw, value, out_gate = jnp.split(relative_scatter_sum(projected), 4, axis=1)

    shape_heads = (seqs, heads, head_size)
    forget = (lower_bound + (1.0 - lower_bound) * jax.nn.sigmoid(forget_raw)).reshape(shape_heads)
    key_in = ((1.0 - lower_bound) * jax.nn.sigmoid(-forget_raw)).reshape(shape_heads)
    query = jax.nn.silu(query_raw).reshape(shape_heads)
    value = value.reshape(shape_heads)
    new_state = forget[..., None] * old_state + key_in[..., None] * value[:, :, None, :]
    read = (
        jnp.sum((query * forget)[..., None] * old_state, axis=2)
        + jnp.sum(query * key_in, axis=2, keepdims=True) * value
    )
    gated = (
        read
        * rms_scale(read)
        * head_gain.reshape(heads, head_size)
        * jax.nn.silu(out_gate).reshape(shape_heads)
    )
    mixed_heads = gated.reshape(seqs, local).astype(BF16)
    mix_part = jnp.stack(
        [
            jnp.dot(mixed_heads, mix_weights[j], preferred_element_type=F32).astype(BF16)
            for j in range(ep_size)
        ],
        axis=1,
    )
    mix_out = relative_to_absolute(sum_over_tp(mix_part).astype(BF16), ep_index)
    mix_wide = mix_out.reshape(seqs, width).astype(F32)
    after_mix = resid + mix_wide * rms_scale(mix_wide) * norm_gains[1]
    ffn_in = (after_mix * rms_scale(after_mix) * norm_gains[2]).astype(BF16)

    first = jax.nn.sigmoid(route_scores[:, 0] - route_scores[:, 1])
    second = jax.nn.sigmoid(route_scores[:, 1] - route_scores[:, 0])
    route_weight = jnp.stack([first, second], axis=1)
    experts = jnp.arange(ep_size, dtype=jnp.int32)
    table = jnp.sum(
        jnp.where(routes[:, :, None] == experts[None, None, :], route_weight[:, :, None], 0.0),
        axis=1,
    )
    mix_weight = jax.nn.sigmoid(
        jnp.sum(ffn_in.astype(F32) * dense_mix.astype(F32), axis=1, keepdims=True)
    )
    extra = jnp.concatenate([table, mix_weight], axis=1)
    high = extra.astype(BF16)
    low = (extra - high.astype(F32)).astype(BF16)
    extra_width = extra.shape[1]
    padding = jnp.zeros((seqs, -(2 * extra_width) % 128), BF16)
    packed = jnp.concatenate([ffn_in, high, low, padding], axis=1)
    gathered = relative_gather(packed).reshape(ep_size * seqs, packed.shape[1])
    rows = gathered[:, :width]
    side = (
        gathered[:, width : width + extra_width].astype(F32)
        + gathered[:, width + extra_width : width + 2 * extra_width].astype(F32)
    )
    expert_scale = lax.dynamic_slice_in_dim(side, ep_index, 1, 1)
    dense_scale = side[:, extra_width - 1 :]

    dense_rows = lax.dynamic_slice_in_dim(rows, ep_index * feats, feats, 1)
    dense_part = jnp.concatenate(
        [
            jnp.dot(dense_rows, w, preferred_element_type=F32)
            for w in (w_dense_gate, w_dense_up)
        ],
        axis=1,
    )
    dense_pre = relative_scatter_sum(dense_part.reshape(ep_size, seqs, -1))
    dense_gate_pre, dense_up_pre = jnp.split(dense_pre, 2, axis=1)
    dense_hidden = (jax.nn.silu(dense_gate_pre) * dense_up_pre).astype(BF16)
    all_hidden = relative_gather(dense_hidden).reshape(ep_size * seqs, -1)
    dense_out = jnp.dot(all_hidden, w_dense_down, preferred_element_type=F32) * dense_scale

    gate_pre = jnp.dot(rows, w_exp_gate[0], preferred_element_type=F32)
    up_pre = jnp.dot(rows, w_exp_up[0], preferred_element_type=F32)
    hidden = (jax.nn.silu(gate_pre) * up_pre).astype(BF16)
    expert_out = jnp.dot(hidden, w_exp_down[0], preferred_element_type=F32) * expert_scale
    mine = (jnp.arange(ep_size, dtype=jnp.int32) == ep_index)[None, :, None]
    out_part = expert_out.reshape(ep_size * seqs, ep_size, feats) + jnp.where(
        mine, dense_out[:, None, :], 0.0
    )
    ffn_part = relative_scatter_sum(out_part.reshape(ep_size, seqs, width))
    ffn_out = sum_over_tp(ffn_part)
    scaled = ffn_out * rms_scale(ffn_out) * norm_gains[3] + after_mix
    layer_out = lax.dynamic_slice_in_dim(scaled, column_index * part_width, part_width, 1)
    return (layer_out.astype(BF16), new_state)


def solution(mesh):
    return jax.shard_map(
        body,
        mesh=mesh,
        in_specs=(
            P("ep", None),
            P("ep", "tp", None, None),
            P("tp"),
            P("tp"),
            P(),
            P("ep", "tp"),
            P("ep", "tp"),
            P("ep", "tp"),
            P("ep", "tp"),
            P("tp", "ep"),
            P("ep", None),
            P("ep", None),
            P("ep", None, "tp"),
            P("ep", None, "tp"),
            P("ep", "tp", None),
            P("ep", "tp"),
            P("ep", "tp"),
            P("tp", "ep"),
            P(),
        ),
        out_specs=(P("ep", "tp"), P("ep", "tp", None, None)),
        check_vma=False,
    )
```

```python
import jax
import jax.numpy as jnp
from jax import lax
from jax.experimental import pallas as pl
from jax.experimental.pallas import tpu as pltpu
from jax.sharding import PartitionSpec as P


EPS = 1e-06
F32 = jnp.float32
BF16 = jnp.bfloat16


def rms_scale(values):
    return lax.rsqrt(jnp.mean(values * values, axis=-1, keepdims=True) + EPS)


def swap(value, axis, step):
    size = lax.axis_size(axis)
    return lax.ppermute(value, axis, [(i, i ^ step) for i in range(size)])


def chip_steps():
    return range(2, lax.axis_size("ep"), 2)


def relative_exchange(even, odd):
    crossed = swap(odd, "ep", 1)
    pairs = jnp.stack([even, crossed], axis=1)
    return [pairs[0]] + [swap(pairs[s // 2], "ep", s) for s in chip_steps()]


def chip_gather(block):
    return [block] + [swap(block, "ep", s) for s in chip_steps()]


def relative_gather(block):
    even = chip_gather(block)
    odd = [swap(item, "ep", 1) for item in even]
    return jnp.stack([item for pair in zip(even, odd) for item in pair])


def chip_send(parts):
    return [swap(part, "ep", s) for part, s in zip(parts, chip_steps())]


def total_of(own, arrived):
    for part in arrived:
        own = own + part.astype(F32)
    return own


def tp_exchange(value):
    return [swap(value, "tp", s) for s in range(1, lax.axis_size("tp"))]


def background_gather(block):
    blocks = [block]
    step = 2
    while step < lax.axis_size("ep"):
        fresh = [swap(block, "ep", step)]
        lower = 2
        while lower < step:
            fresh = fresh + [swap(item, "ep", lower) for item in fresh]
            lower *= 2
        blocks = blocks + fresh
        step *= 2
    odd = [swap(item, "ep", 1) for item in blocks]
    return [item for pair in zip(blocks, odd) for item in pair]


VMEM = pl.BlockSpec(memory_space=pltpu.VMEM)
PARAMS = pltpu.CompilerParams(vmem_limit_bytes=16 << 20)


def call(kernel, out_shape, flops=1 << 20):
    estimate = pl.CostEstimate(flops=flops, bytes_accessed=1 << 20, transcendentals=0)
    return pl.pallas_call(
        kernel, out_shape=out_shape, compiler_params=PARAMS, cost_estimate=estimate
    )


def front_kernel(tokens_ref, gains_ref, even_ref, odd_ref):
    resid = tokens_ref[...].astype(F32)
    chips, _, feats = even_ref.shape
    scale = rms_scale(resid)
    mine = lax.axis_index("ep")
    for j in range(2 * chips):
        cols = pl.ds(pl.multiple_of((mine ^ j) * feats, feats), feats)
        piece = tokens_ref[:, cols].astype(F32) * scale * gains_ref[0:1, cols]
        (odd_ref if j % 2 else even_ref)[j // 2] = piece.astype(BF16)


def front(tokens, norm_gains, ep_size):
    seqs, width = tokens.shape
    feats = width // ep_size
    if feats % 128:
        resid = tokens.astype(F32)
        normed = (resid * rms_scale(resid) * norm_gains[0]).astype(BF16)
        pieces = [
            lax.dynamic_slice_in_dim(normed, (lax.axis_index("ep") ^ j) * feats, feats, 1)
            for j in range(ep_size)
        ]
        return jnp.stack(pieces[::2]), jnp.stack(pieces[1::2])
    shape = jax.ShapeDtypeStruct((ep_size // 2, seqs, width // ep_size), BF16)
    return call(front_kernel, (shape, shape))(tokens, norm_gains)


def project_kernel(pairs, *refs):
    rows_refs, weights = refs[:pairs], refs[pairs:-2]
    keep_ref, send_ref = refs[-2:]
    _, seqs, _ = keep_ref.shape
    feats = weights[0].shape[0]
    rows = jnp.concatenate([ref[...].reshape(2 * seqs, feats) for ref in rows_refs], axis=0)
    start = 0
    for w in weights:
        cols = slice(start, start + w.shape[1])
        part = jnp.dot(rows, w[...], preferred_element_type=F32)
        for s in range(pairs):
            base = 2 * s * seqs
            keep_ref[s, :, cols] = part[base : base + seqs]
            send_ref[s, :, cols] = part[base + seqs : base + 2 * seqs].astype(BF16)
        start = cols.stop


def project(row_pairs, weights):
    chips = len(row_pairs)
    shape = (chips, row_pairs[0].shape[1], sum(w.shape[1] for w in weights))
    return call(
        lambda *refs: project_kernel(chips, *refs),
        (jax.ShapeDtypeStruct(shape, F32), jax.ShapeDtypeStruct(shape, BF16)),
    )(*row_pairs, *weights)


def chip_sum_kernel(keep_ref, crossed_ref, own_ref, *send_refs):
    own_ref[...] = keep_ref[0] + crossed_ref[0].astype(F32)
    for s, ref in enumerate(send_refs):
        ref[...] = (keep_ref[s + 1] + crossed_ref[s + 1].astype(F32)).astype(BF16)


def chip_sum(keep, crossed):
    chips, seqs, width = keep.shape
    sent = jax.ShapeDtypeStruct((seqs, width), BF16)
    out = (jax.ShapeDtypeStruct((seqs, width), F32),) + (sent,) * (chips - 1)
    own, *sends = call(chip_sum_kernel, out)(keep, crossed)
    return own, sends


def mix_kernel(heads_ref, *refs):
    *weights, out_ref = refs
    value = heads_ref[...]
    for j, w in enumerate(weights):
        width = w.shape[1]
        part = jnp.dot(value, w[...], preferred_element_type=F32)
        out_ref[:, j * width : (j + 1) * width] = part.astype(BF16)


def mix_heads(mixed_heads, weights):
    shape = (mixed_heads.shape[0], weights[0].shape[1] * len(weights))
    return call(mix_kernel, jax.ShapeDtypeStruct(shape, BF16))(mixed_heads, *weights)


def middle_kernel(parts, tokens_ref, gains_ref, gate_ref, routes_ref, scores_ref, *refs):
    pieces, (after_ref, packed_ref) = refs[:parts], refs[parts:]
    seqs, width = tokens_ref.shape
    ep_size = lax.axis_size("ep")
    feats = width // ep_size
    mine = lax.axis_index("ep")
    for j in range(ep_size):
        total = pieces[0][:, j * feats : (j + 1) * feats].astype(F32)
        for piece in pieces[1:]:
            total = total + piece[:, j * feats : (j + 1) * feats].astype(F32)
        cols = pl.ds(pl.multiple_of((mine ^ j) * feats, feats), feats)
        after_ref[:, cols] = total.astype(BF16).astype(F32)
    mix_wide = after_ref[...]
    after_mix = tokens_ref[...].astype(F32) + mix_wide * rms_scale(mix_wide) * gains_ref[1:2]
    after_ref[...] = after_mix
    ffn_in = (after_mix * rms_scale(after_mix) * gains_ref[2:3]).astype(BF16)
    packed_ref[:, :width] = ffn_in
    dots = jnp.sum(ffn_in.astype(F32) * gate_ref[...].astype(F32), axis=1, keepdims=True)
    lanes = (packed_ref.shape[1] - width) // 2
    place = lax.broadcasted_iota(jnp.int32, (seqs, lanes), 1)
    extra = jnp.where(place == ep_size, jax.nn.sigmoid(dots), 0.0)
    for k in range(2):
        margin = scores_ref[:, k : k + 1] - scores_ref[:, 1 - k : 2 - k]
        extra = jnp.where(place == routes_ref[:, k : k + 1], jax.nn.sigmoid(margin), extra)
    high = extra.astype(BF16)
    packed_ref[:, width : width + lanes] = high
    packed_ref[:, width + lanes :] = (extra - high.astype(F32)).astype(BF16)


def to_absolute(values, index, ep_size):
    rows, width = values.shape
    values = values.reshape(rows, ep_size, width // ep_size)
    order = index ^ jnp.arange(ep_size, dtype=jnp.int32)
    return jnp.take(values, order, axis=1).reshape(rows, width)


def plain_middle(tokens, norm_gains, dense_mix, routes, route_scores, lanes, pieces):
    ep_size = lax.axis_size("ep")
    total = total_of(pieces[0].astype(F32), pieces[1:])
    mix_wide = to_absolute(total.astype(BF16).astype(F32), lax.axis_index("ep"), ep_size)
    after_mix = tokens.astype(F32) + mix_wide * rms_scale(mix_wide) * norm_gains[1]
    ffn_in = (after_mix * rms_scale(after_mix) * norm_gains[2]).astype(BF16)
    dots = jnp.sum(ffn_in.astype(F32) * dense_mix.astype(F32), axis=1, keepdims=True)
    place = jnp.arange(lanes, dtype=jnp.int32)[None]
    extra = jnp.where(place == ep_size, jax.nn.sigmoid(dots), 0.0)
    for k in range(2):
        margin = route_scores[:, k : k + 1] - route_scores[:, 1 - k : 2 - k]
        extra = jnp.where(place == routes[:, k : k + 1], jax.nn.sigmoid(margin), extra)
    high = extra.astype(BF16)
    low = (extra - high.astype(F32)).astype(BF16)
    return after_mix, jnp.concatenate([ffn_in, high, low], axis=1)


def middle(tokens, norm_gains, dense_mix, routes, route_scores, lanes, pieces):
    seqs, width = tokens.shape
    if (width // lax.axis_size("ep")) % 128:
        return plain_middle(tokens, norm_gains, dense_mix, routes, route_scores, lanes, pieces)
    return call(
        lambda *refs: middle_kernel(len(pieces), *refs),
        (
            jax.ShapeDtypeStruct((seqs, width), F32),
            jax.ShapeDtypeStruct((seqs, width + 2 * lanes), BF16),
        ),
    )(tokens, norm_gains, dense_mix, routes, route_scores, *pieces)


def join_kernel(chips, expert_ref, scale_ref, own_ref, other_ref, *refs):
    hidden, (keep_ref, send_ref) = refs[:chips], refs[chips:]
    _, seqs, _ = keep_ref.shape
    feats = own_ref.shape[1]
    mine = lax.axis_index("ep")
    for s in range(chips):
        rows = 2 * seqs * s
        keep_ref[s] = expert_ref[rows : rows + seqs]
    everything = jnp.concatenate([ref[...] for ref in hidden], axis=0)
    scale = scale_ref[...]
    placed = []
    for weights, column in ((own_ref, mine), (other_ref, mine ^ 1)):
        dense = jnp.dot(everything, weights[...], preferred_element_type=F32) * scale
        cols = pl.ds(pl.multiple_of(column * feats, feats), feats)
        placed.append((cols, dense))
        for s in range(chips):
            rows = 2 * seqs * s
            keep_ref[s, :, cols] += dense[rows : rows + seqs]
    for s in range(chips):
        rows = 2 * seqs * s + seqs
        send_ref[s] = expert_ref[rows : rows + seqs].astype(BF16)
        for cols, dense in placed:
            value = expert_ref[rows : rows + seqs, cols] + dense[rows : rows + seqs]
            send_ref[s, :, cols] = value.astype(BF16)


def plain_join(expert_out, scale, down_own, down_other, hidden, seqs):
    ep_size = lax.axis_size("ep")
    mine = lax.axis_index("ep")
    everything = jnp.concatenate(hidden, axis=0)
    rows, width = expert_out.shape
    total = expert_out.reshape(rows, ep_size, width // ep_size)
    column = jnp.arange(ep_size, dtype=jnp.int32)[None, :, None]
    for weights, place in ((down_own, mine), (down_other, mine ^ 1)):
        dense = jnp.dot(everything, weights, preferred_element_type=F32) * scale
        total = total + jnp.where(column == place, dense[:, None, :], 0.0)
    total = total.reshape(len(hidden), 2, seqs, width)
    return total[:, 0], total[:, 1].astype(BF16)


def join(expert_out, scale, down_own, down_other, hidden, seqs):
    chips, width = len(hidden), expert_out.shape[1]
    shape = (chips, seqs, width)
    if down_own.shape[1] % 128:
        return plain_join(expert_out, scale, down_own, down_other, hidden, seqs)
    return call(
        lambda *refs: join_kernel(chips, *refs),
        (jax.ShapeDtypeStruct(shape, F32), jax.ShapeDtypeStruct(shape, BF16)),
    )(expert_out, scale, down_own, down_other, *hidden)


def finish_kernel(parts, after_ref, gains_ref, *refs):
    pieces, out_ref = refs[:parts], refs[parts]
    total = pieces[0][...].astype(F32)
    for piece in pieces[1:]:
        total = total + piece[...].astype(F32)
    scale = rms_scale(total)
    width = out_ref.shape[1]
    cols = pl.ds(pl.multiple_of(lax.axis_index("tp") * width, width), width)
    mine = pieces[0][:, cols].astype(F32)
    for piece in pieces[1:]:
        mine = mine + piece[:, cols].astype(F32)
    out_ref[...] = (after_ref[:, cols] + mine * scale * gains_ref[3:4, cols]).astype(BF16)


def finish(after_mix, norm_gains, pieces):
    seqs, width = after_mix.shape
    return call(
        lambda *refs: finish_kernel(len(pieces), *refs),
        jax.ShapeDtypeStruct((seqs, width // lax.axis_size("tp")), BF16),
    )(after_mix, norm_gains, *pieces)


def broadcast_column(columns, index, size):
    return jnp.broadcast_to(columns[:, index : index + 1], (size, size))


def read_kernel(arrived, *refs):
    own_ref, recv = refs[0], refs[1 : 1 + arrived]
    bound_ref, gain_ref, state_ref, mixed_ref, gates_ref = refs[1 + arrived :]
    seqs, heads, size, _ = state_ref.shape
    local = heads * size

    def column(kind, head):
        cols = slice(kind * local + head * size, kind * local + (head + 1) * size)
        value = own_ref[:, cols]
        for ref in recv:
            value = value + ref[:, cols].astype(F32)
        return value

    for head in range(heads):
        query_raw, forget_raw, value, out_gate = (column(kind, head) for kind in range(4))
        span = slice(head * size, (head + 1) * size)
        bound = bound_ref[:, span]
        forget = bound + (1.0 - bound) * jax.nn.sigmoid(forget_raw)
        key_in = (1.0 - bound) * jax.nn.sigmoid(-forget_raw)
        query = query_raw * jax.nn.sigmoid(query_raw)
        gates_ref[0, :, span] = forget
        gates_ref[1, :, span] = key_in
        gates_ref[2, :, span] = value
        weight = (query * forget).T
        rows = [
            jnp.sum(
                broadcast_column(weight, t, size) * state_ref[t, head], axis=0, keepdims=True
            )
            for t in range(seqs)
        ]
        read = jnp.concatenate(rows, axis=0)
        read = read + jnp.sum(query * key_in, axis=1, keepdims=True) * value
        gated = read * rms_scale(read) * gain_ref[:, span]
        mixed_ref[:, span] = (gated * (out_gate * jax.nn.sigmoid(out_gate))).astype(BF16)


def read_heads(own, arrived, lower_bound, head_gain, old_state):
    seqs, heads, size, _ = old_state.shape
    return call(
        lambda *refs: read_kernel(len(arrived), *refs),
        (
            jax.ShapeDtypeStruct((seqs, heads * size), BF16),
            jax.ShapeDtypeStruct((3, seqs, heads * size), F32),
        ),
    )(own, *arrived, lower_bound[None], head_gain[None], old_state)


def state_kernel(gates_ref, state_ref, *refs):
    out_ref = refs[-1]
    seqs, size = gates_ref.shape[1:]
    forget = gates_ref[0].T
    key_in = gates_ref[1].T
    for t in range(seqs):
        out_ref[t, 0] = (
            broadcast_column(forget, t, size) * state_ref[t, 0]
            + broadcast_column(key_in, t, size) * gates_ref[2, t : t + 1, :]
        )


def write_state(gates, old_state, first, count, partial=None):
    seqs, _, size, _ = old_state.shape
    block = pl.BlockSpec((seqs, 1, size, size), lambda h: (0, first + h, 0, 0))
    more = () if partial is None else (partial,)
    return pl.pallas_call(
        state_kernel,
        grid=(count,),
        in_specs=[pl.BlockSpec((3, seqs, size), lambda h: (0, 0, first + h)), block]
        + [pl.BlockSpec(memory_space=pl.ANY)] * len(more),
        out_specs=block,
        out_shape=jax.ShapeDtypeStruct(old_state.shape, F32),
        input_output_aliases={2: 0} if more else {},
        compiler_params=PARAMS,
        cost_estimate=pl.CostEstimate(
            flops=4 * old_state.size, bytes_accessed=8 * old_state.size, transcendentals=0
        ),
        name="write_state",
    )(gates, old_state, *more)


def body(
    tokens,
    old_state,
    lower_bound,
    head_gain,
    norm_gains,
    w_query,
    w_forget,
    w_value,
    w_outgate,
    w_mix_out,
    routes,
    route_scores,
    w_exp_gate,
    w_exp_up,
    w_exp_down,
    w_dense_gate,
    w_dense_up,
    w_dense_down,
    dense_mix,
):
    seqs, width = tokens.shape
    ep_index = lax.axis_index("ep")
    core_index = ep_index & 1
    ep_size = lax.axis_size("ep")
    chips = ep_size // 2
    feats = width // ep_size
    all_rows = ep_size * seqs

    mix_weights = background_gather(w_mix_out)

    half_ff = w_dense_gate.shape[1] // 2

    def half(weights, axis, which):
        return lax.dynamic_slice_in_dim(weights, which * half_ff, half_ff, axis)

    other_core = 1 - core_index
    pair = (w_dense_gate, w_dense_up)
    gate_up_out = jnp.concatenate([half(w, 1, other_core) for w in pair], axis=1)
    down_out = half(w_dense_down, 0, other_core)
    gate_up_own = jnp.concatenate([half(w, 1, core_index) for w in pair], axis=1)
    down_own = half(w_dense_down, 0, core_index)
    gate_row = dense_mix.reshape(1, width)
    gate_up_other = swap(gate_up_out, "ep", 1)
    down_other = swap(down_out, "ep", 1)

    lanes = -(-(ep_size + 1) // 128) * 128

    even, odd = front(tokens, norm_gains, ep_size)
    row_pairs = relative_exchange(even, odd)
    keep, send = project(row_pairs, (w_query, w_forget, w_value, w_outgate))
    own, sends = chip_sum(keep, swap(send, "ep", 1))
    arrived = chip_send(sends)
    mixed_heads, gates = read_heads(own, arrived, lower_bound, head_gain, old_state)
    heads = old_state.shape[1]
    early = -(-heads // 2)
    new_state = write_state(gates, old_state, 0, early)
    if heads > early:
        new_state = write_state(gates, old_state, early, heads - early, new_state)
    mix_part = mix_heads(mixed_heads, mix_weights)
    mix_pieces = [mix_part] + tp_exchange(mix_part)
    after_mix, packed = middle(
        tokens, norm_gains, gate_row, routes, route_scores, lanes, mix_pieces
    )

    gathered = relative_gather(packed).reshape(all_rows, packed.shape[1])
    rows = gathered[:, :width]
    side = gathered[:, width : width + lanes].astype(F32) + gathered[:, width + lanes :].astype(F32)
    expert_scale = lax.dynamic_slice_in_dim(side, ep_index, 1, 1)
    dense_scale = side[:, ep_size : ep_size + 1]

    def features(index):
        return lax.dynamic_slice_in_dim(rows, index * feats, feats, 1)

    dense_part = jnp.dot(features(ep_index), gate_up_own, preferred_element_type=F32) + jnp.dot(
        features(ep_index ^ 1), gate_up_other, preferred_element_type=F32
    )
    dense_part = dense_part.reshape(chips, 2 * seqs, -1)
    dense_sent = dense_part[1:].astype(BF16)
    dense_pre = total_of(dense_part[0], chip_send(list(dense_sent)))
    dense_gate_pre, dense_up_pre = jnp.split(dense_pre, 2, axis=1)
    dense_hidden = (jax.nn.silu(dense_gate_pre) * dense_up_pre).astype(BF16)
    all_hidden = chip_gather(dense_hidden)

    gate_pre = jnp.dot(rows, w_exp_gate[0], preferred_element_type=F32)
    gate_pre = lax.optimization_barrier(gate_pre)
    up_pre = jnp.dot(rows, w_exp_up[0], preferred_element_type=F32)
    hidden = (jax.nn.silu(gate_pre) * up_pre).astype(BF16)
    hidden = lax.optimization_barrier(hidden)
    expert_out = jnp.dot(hidden, w_exp_down[0], preferred_element_type=F32) * expert_scale
    expert_out = lax.optimization_barrier(expert_out)
    keep, send = join(expert_out, dense_scale, down_own, down_other, all_hidden, seqs)
    own, sends = chip_sum(keep, swap(send, "ep", 1))
    ffn_part = total_of(own, chip_send(sends)).astype(BF16)
    ffn_pieces = [ffn_part] + tp_exchange(ffn_part)
    return (finish(after_mix, norm_gains, ffn_pieces), new_state)


def solution(mesh):
    return jax.shard_map(
        body,        mesh=mesh,
        in_specs=(
            P("ep", None),
            P("ep", "tp", None, None),
            P("tp"),
            P("tp"),
            P(),
            P("ep", "tp"),
            P("ep", "tp"),
            P("ep", "tp"),
            P("ep", "tp"),
            P("tp", "ep"),
            P("ep", None),
            P("ep", None),
            P("ep", None, "tp"),
            P("ep", None, "tp"),
            P("ep", "tp", None),
            P("ep", "tp"),
            P("ep", "tp"),
            P("tp", "ep"),
            P(),
        ),
        out_specs=(P("ep", "tp"), P("ep", "tp", None, None)),
        check_vma=False,
    )
```

```python
import jax
import jax.numpy as jnp
from jax import lax
from jax.experimental import pallas as pl
from jax.experimental.pallas import tpu as pltpu
from jax.sharding import PartitionSpec as P


EPS = 1e-06
F32 = jnp.float32
BF16 = jnp.bfloat16


def rms_scale(values):
    return lax.rsqrt(jnp.mean(values * values, axis=-1, keepdims=True) + EPS)


def swap(value, axis, step):
    size = lax.axis_size(axis)
    return lax.ppermute(value, axis, [(i, i ^ step) for i in range(size)])


def chip_steps():
    return range(2, lax.axis_size("ep"), 2)


def relative_exchange(even, odd):
    crossed = swap(odd, "ep", 1)
    pairs = jnp.stack([even, crossed], axis=1)
    return [pairs[0]] + [swap(pairs[s // 2], "ep", s) for s in chip_steps()]


def chip_gather(block):
    return [block] + [swap(block, "ep", s) for s in chip_steps()]


def pair_gather(block):
    even = chip_gather(block)
    return [(item, swap(item, "ep", 1)) for item in even]


def chip_send(parts):
    return [swap(part, "ep", s) for part, s in zip(parts, chip_steps())]


def total_of(own, arrived):
    for part in arrived:
        own = own + part.astype(F32)
    return own


def tp_exchange(value):
    return [swap(value, "tp", s) for s in range(1, lax.axis_size("tp"))]


def background_gather(block):
    blocks = [block]
    step = 2
    while step < lax.axis_size("ep"):
        fresh = [swap(block, "ep", step)]
        lower = 2
        while lower < step:
            fresh = fresh + [swap(item, "ep", lower) for item in fresh]
            lower *= 2
        blocks = blocks + fresh
        step *= 2
    odd = [swap(item, "ep", 1) for item in blocks]
    return [item for pair in zip(blocks, odd) for item in pair]


VMEM = pl.BlockSpec(memory_space=pltpu.VMEM)
FAR = pl.BlockSpec(memory_space=pltpu.HBM)


def far(*values):
    return tuple(pltpu.with_memory_space_constraint(value, pltpu.HBM) for value in values)


def near(values):
    return [pltpu.with_memory_space_constraint(value, pltpu.VMEM) for value in values]


def fetch(sources, targets, sems):
    copies = [
        pltpu.make_async_copy(source, target, sems.at[i])
        for i, (source, target) in enumerate(zip(sources, targets))
    ]
    for copy in copies:
        copy.start()
    for copy in copies:
        copy.wait()


PARAMS = pltpu.CompilerParams(vmem_limit_bytes=16 << 20)


def call(kernel, out_shape, flops=1 << 20):
    estimate = pl.CostEstimate(flops=flops, bytes_accessed=1 << 20, transcendentals=0)
    return pl.pallas_call(
        kernel, out_shape=out_shape, compiler_params=PARAMS, cost_estimate=estimate
    )


def front_kernel(tokens_in, gains_in, bound_in, gain_in, even_ref, odd_ref, tokens_ref, gains_ref, heads_ref, sems):
    targets = (tokens_ref, gains_ref, heads_ref.at[0:1], heads_ref.at[1:2])
    fetch((tokens_in, gains_in, bound_in, gain_in), targets, sems)
    chips, _, feats = even_ref.shape
    scale = rms_scale(tokens_ref[...].astype(F32))
    mine = lax.axis_index("ep")
    for j in range(2 * chips):
        cols = pl.ds(pl.multiple_of((mine ^ j) * feats, feats), feats)
        piece = tokens_ref[:, cols].astype(F32) * scale * gains_ref[0:1, cols]
        (odd_ref if j % 2 else even_ref)[j // 2] = piece.astype(BF16)


def front(tokens, norm_gains, lower_bound, head_gain, ep_size):
    seqs, width = tokens.shape
    feats = width // ep_size
    if feats % 128:
        resid = tokens.astype(F32)
        normed = (resid * rms_scale(resid) * norm_gains[0]).astype(BF16)
        pieces = [
            lax.dynamic_slice_in_dim(normed, (lax.axis_index("ep") ^ j) * feats, feats, 1)
            for j in range(ep_size)
        ]
        head_rows = jnp.stack([lower_bound, head_gain])
        return jnp.stack(pieces[::2]), jnp.stack(pieces[1::2]), tokens, norm_gains, head_rows
    shape = jax.ShapeDtypeStruct((ep_size // 2, seqs, feats), BF16)
    return pl.pallas_call(
        front_kernel,
        in_specs=[FAR] * 4,
        out_shape=(
            shape,
            shape,
            jax.ShapeDtypeStruct(tokens.shape, tokens.dtype),
            jax.ShapeDtypeStruct(norm_gains.shape, F32),
            jax.ShapeDtypeStruct((2, lower_bound.shape[0]), F32),
        ),
        scratch_shapes=[pltpu.SemaphoreType.DMA((4,))],
        compiler_params=PARAMS,
        name="front",
    )(*far(tokens, norm_gains, lower_bound[None], head_gain[None]))


def table_kernel(routes_in, scores_in, gate_in, table_ref, gate_ref, routes_ref, scores_ref, sems):
    fetch((routes_in, scores_in, gate_in), (routes_ref, scores_ref, gate_ref), sems)
    seqs = table_ref.shape[0]
    place = lax.broadcasted_iota(jnp.int32, table_ref.shape, 1)
    across = lax.broadcasted_iota(jnp.int32, (seqs, seqs), 1)
    diagonal = across == lax.broadcasted_iota(jnp.int32, (seqs, seqs), 0)

    def upright(row):
        return jnp.sum(jnp.where(diagonal, row, 0.0), axis=1, keepdims=True)

    table = jnp.zeros(table_ref.shape, F32)
    for k in range(2):
        margin = scores_ref[k : k + 1, :] - scores_ref[1 - k : 2 - k, :]
        expert = upright(routes_ref[k : k + 1, :].astype(F32)).astype(jnp.int32)
        table = jnp.where(place == expert, upright(jax.nn.sigmoid(margin)), table)
    table_ref[...] = table


def route_table(routes, route_scores, dense_mix, lanes):
    shape = jax.ShapeDtypeStruct((routes.shape[0], lanes), F32)
    gate = dense_mix.reshape(-1, 128)
    shapes = (shape, jax.ShapeDtypeStruct(gate.shape, gate.dtype))
    operands = (routes.T, route_scores.T, gate)
    return pl.pallas_call(
        table_kernel,
        in_specs=[FAR] * 3,
        out_shape=shapes,
        scratch_shapes=[pltpu.VMEM(x.shape, x.dtype) for x in operands[:2]]
        + [pltpu.SemaphoreType.DMA((3,))],
        compiler_params=PARAMS,
        cost_estimate=pl.CostEstimate(flops=1 << 34, bytes_accessed=1 << 20, transcendentals=0),
        name="table",
    )(*far(*operands))


def project_kernel(pairs, *refs):
    rows_refs, weights = refs[:pairs], refs[pairs:-2]
    keep_ref, send_ref = refs[-2:]
    _, seqs, _ = keep_ref.shape
    feats = weights[0].shape[0]
    rows = jnp.concatenate([ref[...].reshape(2 * seqs, feats) for ref in rows_refs], axis=0)
    start = 0
    for w in weights:
        cols = slice(start, start + w.shape[1])
        part = jnp.dot(rows, w[...], preferred_element_type=F32)
        for s in range(pairs):
            base = 2 * s * seqs
            keep_ref[s, :, cols] = part[base : base + seqs]
            send_ref[s, :, cols] = part[base + seqs : base + 2 * seqs].astype(BF16)
        start = cols.stop


def project(row_pairs, weights):
    chips = len(row_pairs)
    shape = (chips, row_pairs[0].shape[1], sum(w.shape[1] for w in weights))
    return call(
        lambda *refs: project_kernel(chips, *refs),
        (jax.ShapeDtypeStruct(shape, F32), jax.ShapeDtypeStruct(shape, BF16)),
    )(*row_pairs, *weights)


def chip_sum_kernel(keep_ref, crossed_ref, own_ref, *send_refs):
    own_ref[...] = keep_ref[0] + crossed_ref[0].astype(F32)
    for s, ref in enumerate(send_refs):
        ref[...] = (keep_ref[s + 1] + crossed_ref[s + 1].astype(F32)).astype(BF16)


def chip_sum(keep, crossed):
    chips, seqs, width = keep.shape
    sent = jax.ShapeDtypeStruct((seqs, width), BF16)
    out = (jax.ShapeDtypeStruct((seqs, width), F32),) + (sent,) * (chips - 1)
    own, *sends = call(chip_sum_kernel, out)(keep, crossed)
    return own, sends


def mix_kernel(heads_ref, *refs):
    *weights, out_ref = refs
    value = heads_ref[...]
    for j, w in enumerate(weights):
        width = w.shape[1]
        part = jnp.dot(value, w[...], preferred_element_type=F32)
        out_ref[:, j * width : (j + 1) * width] = part.astype(BF16)


def mix_heads(mixed_heads, weights):
    shape = (mixed_heads.shape[0], weights[0].shape[1] * len(weights))
    return call(mix_kernel, jax.ShapeDtypeStruct(shape, BF16))(mixed_heads, *weights)


def middle_kernel(parts, tokens_ref, gains_ref, gate_ref, table_ref, *refs):
    pieces, (after_ref, packed_ref) = refs[:parts], refs[parts:]
    seqs, width = tokens_ref.shape
    ep_size = lax.axis_size("ep")
    feats = width // ep_size
    mine = lax.axis_index("ep")
    for j in range(ep_size):
        total = pieces[0][:, j * feats : (j + 1) * feats].astype(F32)
        for piece in pieces[1:]:
            total = total + piece[:, j * feats : (j + 1) * feats].astype(F32)
        cols = pl.ds(pl.multiple_of((mine ^ j) * feats, feats), feats)
        after_ref[:, cols] = total.astype(BF16).astype(F32)
    mix_wide = after_ref[...]
    after_mix = tokens_ref[...].astype(F32) + mix_wide * rms_scale(mix_wide) * gains_ref[1:2]
    after_ref[...] = after_mix
    ffn_in = (after_mix * rms_scale(after_mix) * gains_ref[2:3]).astype(BF16)
    packed_ref[:, :width] = ffn_in
    lanes = table_ref.shape[1]
    products = jnp.zeros((seqs, 128), F32)
    for j in range(width // 128):
        piece = packed_ref[:, j * 128 : (j + 1) * 128].astype(F32)
        products = products + piece * gate_ref[j : j + 1, :].astype(F32)
    dots = jnp.sum(products, axis=1, keepdims=True)
    place = lax.broadcasted_iota(jnp.int32, (seqs, lanes), 1)
    extra = jnp.where(place == ep_size, jax.nn.sigmoid(dots), table_ref[...])
    high = extra.astype(BF16)
    packed_ref[:, width : width + lanes] = high
    packed_ref[:, width + lanes :] = (extra - high.astype(F32)).astype(BF16)


def to_absolute(values, index, ep_size):
    rows, width = values.shape
    values = values.reshape(rows, ep_size, width // ep_size)
    order = index ^ jnp.arange(ep_size, dtype=jnp.int32)
    return jnp.take(values, order, axis=1).reshape(rows, width)


def plain_middle(tokens, norm_gains, dense_mix, table, pieces):
    ep_size = lax.axis_size("ep")
    total = total_of(pieces[0].astype(F32), pieces[1:])
    mix_wide = to_absolute(total.astype(BF16).astype(F32), lax.axis_index("ep"), ep_size)
    after_mix = tokens.astype(F32) + mix_wide * rms_scale(mix_wide) * norm_gains[1]
    ffn_in = (after_mix * rms_scale(after_mix) * norm_gains[2]).astype(BF16)
    dots = jnp.sum(ffn_in.astype(F32) * dense_mix.reshape(1, -1).astype(F32), axis=1, keepdims=True)
    place = jnp.arange(table.shape[1], dtype=jnp.int32)[None]
    extra = jnp.where(place == ep_size, jax.nn.sigmoid(dots), table)
    high = extra.astype(BF16)
    low = (extra - high.astype(F32)).astype(BF16)
    return after_mix, jnp.concatenate([ffn_in, high, low], axis=1)


def middle(tokens, norm_gains, dense_mix, table, pieces):
    seqs, width = tokens.shape
    lanes = table.shape[1]
    if (width // lax.axis_size("ep")) % 128:
        return plain_middle(tokens, norm_gains, dense_mix, table, pieces)
    return call(
        lambda *refs: middle_kernel(len(pieces), *refs),
        (
            jax.ShapeDtypeStruct((seqs, width), F32),
            jax.ShapeDtypeStruct((seqs, width + 2 * lanes), BF16),
        ),
    )(tokens, norm_gains, dense_mix, table, *near(pieces))


def dense_kernel(feats, even_ref, odd_ref, *refs):
    *weights, out_ref = refs
    half = out_ref.shape[1] // 2
    mine = lax.axis_index("ep")
    units = pl.ds(pl.multiple_of((mine & 1) * half, half), half)

    def features(index):
        cols = pl.ds(pl.multiple_of(index * feats, feats), feats)
        return jnp.concatenate([even_ref[:, cols], odd_ref[:, cols]], axis=0)

    own, other = features(mine), features(mine ^ 1)
    for k in range(2):
        part = jnp.dot(own, weights[k][:, units], preferred_element_type=F32) + jnp.dot(
            other, weights[2 + k][:, units], preferred_element_type=F32
        )
        out_ref[:, k * half : (k + 1) * half] = part.astype(out_ref.dtype)


def dense_part(even, odd, weights, dtype):
    feats, units = weights[0].shape
    half = units // 2
    if half % 128 or feats % 128:
        mine = lax.axis_index("ep")
        rows = jnp.concatenate([even, odd], axis=0)
        own, other = (
            lax.dynamic_slice_in_dim(rows, index * feats, feats, 1) for index in (mine, mine ^ 1)
        )
        picked = [lax.dynamic_slice_in_dim(w, (mine & 1) * half, half, 1) for w in weights]
        parts = [
            jnp.dot(own, picked[k], preferred_element_type=F32)
            + jnp.dot(other, picked[2 + k], preferred_element_type=F32)
            for k in range(2)
        ]
        return jnp.concatenate(parts, axis=1).astype(dtype)
    return call(
        lambda *refs: dense_kernel(feats, *refs),
        jax.ShapeDtypeStruct((2 * even.shape[0], units), dtype),
    )(even, odd, *weights)


def join_kernel(first, expert_ref, scale_ref, own_ref, other_ref, hidden_ref, keep_ref, send_ref):
    seqs = keep_ref.shape[0]
    half = own_ref.shape[0] // 2
    feats = own_ref.shape[1]
    mine = lax.axis_index("ep")
    units = pl.ds(pl.multiple_of((mine & 1) * half, half), half)
    rows = slice(first, first + seqs)
    others = slice(first + seqs, first + 2 * seqs)
    keep_ref[...] = expert_ref[rows]
    send_ref[...] = expert_ref[others].astype(BF16)
    scale = scale_ref[first : first + 2 * seqs]
    for weights, column in ((own_ref, mine), (other_ref, mine ^ 1)):
        dense = jnp.dot(hidden_ref[...], weights[units, :], preferred_element_type=F32) * scale
        cols = pl.ds(pl.multiple_of(column * feats, feats), feats)
        keep_ref[:, cols] += dense[:seqs]
        send_ref[:, cols] = (expert_ref[others, cols] + dense[seqs:]).astype(BF16)


def plain_join(rows, scale, down_own, down_other, hidden, seqs):
    ep_size = lax.axis_size("ep")
    mine = lax.axis_index("ep")
    count, width = rows.shape
    total = rows.reshape(count, ep_size, width // ep_size)
    column = jnp.arange(ep_size, dtype=jnp.int32)[None, :, None]
    for weights, place in ((down_own, mine), (down_other, mine ^ 1)):
        half = weights.shape[0] // 2
        picked = lax.dynamic_slice_in_dim(weights, (mine & 1) * half, half, 0)
        dense = jnp.dot(hidden, picked, preferred_element_type=F32) * scale
        total = total + jnp.where(column == place, dense[:, None, :], 0.0)
    total = total.reshape(count, width)
    return total[:seqs], total[seqs:].astype(BF16)


def join(expert_out, scale, down_own, down_other, hidden, chip, seqs):
    first = 2 * seqs * chip
    if down_own.shape[1] % 128:
        rows = slice(first, first + 2 * seqs)
        return plain_join(expert_out[rows], scale[rows], down_own, down_other, hidden, seqs)
    shape = (seqs, expert_out.shape[1])
    return call(
        lambda *refs: join_kernel(first, *refs),
        (jax.ShapeDtypeStruct(shape, F32), jax.ShapeDtypeStruct(shape, BF16)),
    )(expert_out, scale, down_own, down_other, hidden)


def core_sum_kernel(keep_ref, crossed_ref, out_ref):
    out_ref[...] = (keep_ref[...] + crossed_ref[...].astype(F32)).astype(out_ref.dtype)


def core_sum(keep, crossed, dtype):
    return call(core_sum_kernel, jax.ShapeDtypeStruct(keep.shape, dtype))(keep, crossed)


def finish_kernel(parts, after_ref, gains_ref, *refs):
    pieces, out_ref = refs[:parts], refs[parts]
    total = pieces[0][...].astype(F32)
    for piece in pieces[1:]:
        total = total + piece[...].astype(F32)
    scale = rms_scale(total)
    width = out_ref.shape[1]
    cols = pl.ds(pl.multiple_of(lax.axis_index("tp") * width, width), width)
    mine = pieces[0][:, cols].astype(F32)
    for piece in pieces[1:]:
        mine = mine + piece[:, cols].astype(F32)
    out_ref[...] = (after_ref[:, cols] + mine * scale * gains_ref[3:4, cols]).astype(BF16)


def finish(after_mix, norm_gains, pieces):
    seqs, width = after_mix.shape
    return call(
        lambda *refs: finish_kernel(len(pieces), *refs),
        jax.ShapeDtypeStruct((seqs, width // lax.axis_size("tp")), BF16),
    )(*near([after_mix, norm_gains, *pieces]))


def broadcast_column(columns, index, size):
    return jnp.broadcast_to(columns[:, index : index + 1], (size, size))


def read_kernel(arrived, *refs):
    own_ref, recv = refs[0], refs[1 : 1 + arrived]
    rows_ref, state_ref, mixed_ref, gates_ref = refs[1 + arrived :]
    seqs, heads, size, _ = state_ref.shape
    local = heads * size

    def column(kind, head):
        cols = slice(kind * local + head * size, kind * local + (head + 1) * size)
        value = own_ref[:, cols]
        for ref in recv:
            value = value + ref[:, cols].astype(F32)
        return value

    for head in range(heads):
        query_raw, forget_raw, value, out_gate = (column(kind, head) for kind in range(4))
        span = slice(head * size, (head + 1) * size)
        bound = rows_ref[0:1, span]
        forget = bound + (1.0 - bound) * jax.nn.sigmoid(forget_raw)
        key_in = (1.0 - bound) * jax.nn.sigmoid(-forget_raw)
        query = query_raw * jax.nn.sigmoid(query_raw)
        gates_ref[0, :, span] = forget
        gates_ref[1, :, span] = key_in
        gates_ref[2, :, span] = value
        weight = (query * forget).T
        rows = [
            jnp.sum(
                broadcast_column(weight, t, size) * state_ref[t, head], axis=0, keepdims=True
            )
            for t in range(seqs)
        ]
        read = jnp.concatenate(rows, axis=0)
        read = read + jnp.sum(query * key_in, axis=1, keepdims=True) * value
        gated = read * rms_scale(read) * rows_ref[1:2, span]
        mixed_ref[:, span] = (gated * (out_gate * jax.nn.sigmoid(out_gate))).astype(BF16)


def read_heads(own, arrived, head_rows, old_state):
    seqs, heads, size, _ = old_state.shape
    return call(
        lambda *refs: read_kernel(len(arrived), *refs),
        (
            jax.ShapeDtypeStruct((seqs, heads * size), BF16),
            jax.ShapeDtypeStruct((3, seqs, heads * size), F32),
        ),
    )(*near([own, *arrived, head_rows]), old_state)


def state_kernel(gates_ref, state_ref, *refs):
    out_ref = refs[-1]
    seqs, size = gates_ref.shape[1:]
    forget = gates_ref[0].T
    key_in = gates_ref[1].T
    for t in range(seqs):
        out_ref[t, 0] = (
            broadcast_column(forget, t, size) * state_ref[t, 0]
            + broadcast_column(key_in, t, size) * gates_ref[2, t : t + 1, :]
        )


def write_state(gates, old_state, first, count, partial=None):
    seqs, _, size, _ = old_state.shape
    block = pl.BlockSpec((seqs, 1, size, size), lambda h: (0, first + h, 0, 0))
    more = () if partial is None else (partial,)
    return pl.pallas_call(
        state_kernel,
        grid=(count,),
        in_specs=[pl.BlockSpec((3, seqs, size), lambda h: (0, 0, first + h)), block]
        + [pl.BlockSpec(memory_space=pl.ANY)] * len(more),
        out_specs=block,
        out_shape=jax.ShapeDtypeStruct(old_state.shape, F32),
        input_output_aliases={2: 0} if more else {},
        compiler_params=PARAMS,
        cost_estimate=pl.CostEstimate(
            flops=4 * old_state.size, bytes_accessed=8 * old_state.size, transcendentals=0
        ),
        name="write_state",
    )(gates, *(far(old_state) if partial is None else (old_state,)), *more)


def body(
    tokens,
    old_state,
    lower_bound,
    head_gain,
    norm_gains,
    w_query,
    w_forget,
    w_value,
    w_outgate,
    w_mix_out,
    routes,
    route_scores,
    w_exp_gate,
    w_exp_up,
    w_exp_down,
    w_dense_gate,
    w_dense_up,
    w_dense_down,
    dense_mix,
):
    seqs, width = tokens.shape
    ep_index = lax.axis_index("ep")
    ep_size = lax.axis_size("ep")

    mix_weights = background_gather(w_mix_out)

    dense_weights = (w_dense_gate, w_dense_up) + tuple(
        swap(w, "ep", 1) for w in (w_dense_gate, w_dense_up)
    )
    down_other = swap(w_dense_down, "ep", 1)
    lanes = -(-(ep_size + 1) // 128) * 128

    table, gate = route_table(routes, route_scores, dense_mix, lanes)
    even, odd, tokens, norm_gains, head_rows = front(
        tokens, norm_gains, lower_bound, head_gain, ep_size
    )
    row_pairs = relative_exchange(even, odd)
    keep, send = project(row_pairs, (w_query, w_forget, w_value, w_outgate))
    own, sends = chip_sum(keep, swap(send, "ep", 1))
    arrived = chip_send(sends)
    mixed_heads, gates = read_heads(own, arrived, head_rows, old_state)
    heads = old_state.shape[1]
    early = -(-heads // 2)
    new_state = write_state(gates, old_state, 0, early)
    if heads > early:
        new_state = write_state(gates, old_state, early, heads - early, new_state)
    mix_part = mix_heads(mixed_heads, mix_weights)
    mix_pieces = [mix_part] + tp_exchange(mix_part)
    after_mix, packed = middle(tokens, norm_gains, gate, table, mix_pieces)

    row_pairs = pair_gather(packed)
    dense_parts = []
    for s, (even, odd) in enumerate(row_pairs):
        dense_parts.append(dense_part(even, odd, dense_weights, BF16 if s else F32))
    dense_pre = total_of(dense_parts[0], chip_send(dense_parts[1:]))

    gathered = jnp.concatenate([item for pair in row_pairs for item in pair], axis=0)
    rows = gathered[:, :width]
    side = gathered[:, width : width + lanes].astype(F32) + gathered[:, width + lanes :].astype(F32)
    expert_scale = lax.dynamic_slice_in_dim(side, ep_index, 1, 1)
    dense_scale = side[:, ep_size : ep_size + 1]

    dense_gate_pre, dense_up_pre = jnp.split(dense_pre, 2, axis=1)
    dense_hidden = (jax.nn.silu(dense_gate_pre) * dense_up_pre).astype(BF16)
    all_hidden = chip_gather(dense_hidden)

    gate_pre = jnp.dot(rows, w_exp_gate[0], preferred_element_type=F32)
    gate_pre = lax.optimization_barrier(gate_pre)
    up_pre = jnp.dot(rows, w_exp_up[0], preferred_element_type=F32)
    hidden = (jax.nn.silu(gate_pre) * up_pre).astype(BF16)
    hidden = lax.optimization_barrier(hidden)
    expert_out = jnp.dot(hidden, w_exp_down[0], preferred_element_type=F32) * expert_scale
    expert_out = lax.optimization_barrier(expert_out)
    sums = []
    for chip, hidden_rows in enumerate(all_hidden):
        keep, send = join(
            expert_out, dense_scale, w_dense_down, down_other, hidden_rows, chip, seqs
        )
        sums.append(core_sum(keep, swap(send, "ep", 1), BF16 if chip else F32))
    ffn_part = total_of(sums[0], chip_send(sums[1:])).astype(BF16)
    ffn_pieces = [ffn_part] + tp_exchange(ffn_part)
    return (finish(after_mix, norm_gains, ffn_pieces), new_state)


def solution(mesh):
    return jax.shard_map(
        body,        mesh=mesh,
        in_specs=(
            P("ep", None),
            P("ep", "tp", None, None),
            P("tp"),
            P("tp"),
            P(),
            P("ep", "tp"),
            P("ep", "tp"),
            P("ep", "tp"),
            P("ep", "tp"),
            P("tp", "ep"),
            P("ep", None),
            P("ep", None),
            P("ep", None, "tp"),
            P("ep", None, "tp"),
            P("ep", "tp", None),
            P("ep", "tp"),
            P("ep", "tp"),
            P("tp", "ep"),
            P(),
        ),
        out_specs=(P("ep", "tp"), P("ep", "tp", None, None)),
        check_vma=False,
    )
```

```python
import jax
import jax.numpy as jnp
from jax import lax
from jax.experimental import pallas as pl
from jax.experimental.pallas import tpu as pltpu
from jax.sharding import PartitionSpec as P


EPS = 1e-06
F32 = jnp.float32
BF16 = jnp.bfloat16


def rms_scale(values):
    return lax.rsqrt(jnp.mean(values * values, axis=-1, keepdims=True) + EPS)


def swap(value, axis, step):
    size = lax.axis_size(axis)
    return lax.ppermute(value, axis, [(i, i ^ step) for i in range(size)])


def chip_steps():
    return range(2, lax.axis_size("ep"), 2)


def relative_exchange(even, odd):
    crossed = swap(odd, "ep", 1)
    pairs = jnp.stack([even, crossed], axis=1)
    return [pairs[0]] + [swap(pairs[s // 2], "ep", s) for s in chip_steps()]


def chip_gather(block):
    return [block] + [swap(block, "ep", s) for s in chip_steps()]


def pair_gather(block):
    even = chip_gather(block)
    return [(item, swap(item, "ep", 1)) for item in even]


def chip_send(parts):
    return [swap(part, "ep", s) for part, s in zip(parts, chip_steps())]


def total_of(own, arrived):
    for part in arrived:
        own = own + part.astype(F32)
    return own


def tp_exchange(value):
    return [swap(value, "tp", s) for s in range(1, lax.axis_size("tp"))]


def background_gather(block):
    blocks = [block]
    step = 2
    while step < lax.axis_size("ep"):
        fresh = [swap(block, "ep", step)]
        lower = 2
        while lower < step:
            fresh = fresh + [swap(item, "ep", lower) for item in fresh]
            lower *= 2
        blocks = blocks + fresh
        step *= 2
    odd = [swap(item, "ep", 1) for item in blocks]
    return [item for pair in zip(blocks, odd) for item in pair]


VMEM = pl.BlockSpec(memory_space=pltpu.VMEM)
FAR = pl.BlockSpec(memory_space=pltpu.HBM)


def far(*values):
    return tuple(pltpu.with_memory_space_constraint(value, pltpu.HBM) for value in values)


def near(values):
    return [pltpu.with_memory_space_constraint(value, pltpu.VMEM) for value in values]


def fetch(sources, targets, sems):
    copies = [
        pltpu.make_async_copy(source, target, sems.at[i])
        for i, (source, target) in enumerate(zip(sources, targets))
    ]
    for copy in copies:
        copy.start()
    for copy in copies:
        copy.wait()


PARAMS = pltpu.CompilerParams(vmem_limit_bytes=16 << 20)


def call(kernel, out_shape, flops=1 << 20):
    estimate = pl.CostEstimate(flops=flops, bytes_accessed=1 << 20, transcendentals=0)
    return pl.pallas_call(
        kernel, out_shape=out_shape, compiler_params=PARAMS, cost_estimate=estimate
    )


def front_kernel(tokens_in, gains_in, bound_in, gain_in, even_ref, odd_ref, tokens_ref, gains_ref, heads_ref, sems):
    targets = (tokens_ref, gains_ref, heads_ref.at[0:1], heads_ref.at[1:2])
    fetch((tokens_in, gains_in, bound_in, gain_in), targets, sems)
    chips, _, feats = even_ref.shape
    scale = rms_scale(tokens_ref[...].astype(F32))
    mine = lax.axis_index("ep")
    for j in range(2 * chips):
        cols = pl.ds(pl.multiple_of((mine ^ j) * feats, feats), feats)
        piece = tokens_ref[:, cols].astype(F32) * scale * gains_ref[0:1, cols]
        (odd_ref if j % 2 else even_ref)[j // 2] = piece.astype(BF16)


def front(tokens, norm_gains, lower_bound, head_gain, ep_size):
    seqs, width = tokens.shape
    feats = width // ep_size
    if feats % 128:
        resid = tokens.astype(F32)
        normed = (resid * rms_scale(resid) * norm_gains[0]).astype(BF16)
        pieces = [
            lax.dynamic_slice_in_dim(normed, (lax.axis_index("ep") ^ j) * feats, feats, 1)
            for j in range(ep_size)
        ]
        head_rows = jnp.stack([lower_bound, head_gain])
        return jnp.stack(pieces[::2]), jnp.stack(pieces[1::2]), tokens, norm_gains, head_rows
    shape = jax.ShapeDtypeStruct((ep_size // 2, seqs, feats), BF16)
    return pl.pallas_call(
        front_kernel,
        in_specs=[FAR] * 4,
        out_shape=(
            shape,
            shape,
            jax.ShapeDtypeStruct(tokens.shape, tokens.dtype),
            jax.ShapeDtypeStruct(norm_gains.shape, F32),
            jax.ShapeDtypeStruct((2, lower_bound.shape[0]), F32),
        ),
        scratch_shapes=[pltpu.SemaphoreType.DMA((4,))],
        compiler_params=PARAMS,
        name="front",
    )(*far(tokens, norm_gains, lower_bound[None], head_gain[None]))


def table_kernel(routes_in, scores_in, gate_in, table_ref, gate_ref, routes_ref, scores_ref, sems):
    fetch((routes_in, scores_in, gate_in), (routes_ref, scores_ref, gate_ref), sems)
    seqs = table_ref.shape[0]
    low = lax.axis_size("ep") + 1
    place = lax.broadcasted_iota(jnp.int32, table_ref.shape, 1)
    across = lax.broadcasted_iota(jnp.int32, (seqs, seqs), 1)
    diagonal = across == lax.broadcasted_iota(jnp.int32, (seqs, seqs), 0)

    def upright(row):
        return jnp.sum(jnp.where(diagonal, row, 0.0), axis=1, keepdims=True)

    table = jnp.zeros(table_ref.shape, F32)
    for k in range(2):
        margin = scores_ref[k : k + 1, :] - scores_ref[1 - k : 2 - k, :]
        expert = upright(routes_ref[k : k + 1, :].astype(F32)).astype(jnp.int32)
        picked = (place == expert) | (place == expert + low)
        table = jnp.where(picked, upright(jax.nn.sigmoid(margin)), table)
    table_ref[...] = table


def route_table(routes, route_scores, dense_mix, lanes):
    shape = jax.ShapeDtypeStruct((routes.shape[0], lanes), F32)
    gate = dense_mix.reshape(-1, 128)
    shapes = (shape, jax.ShapeDtypeStruct(gate.shape, gate.dtype))
    operands = (routes.T, route_scores.T, gate)
    return pl.pallas_call(
        table_kernel,
        in_specs=[FAR] * 3,
        out_shape=shapes,
        scratch_shapes=[pltpu.VMEM(x.shape, x.dtype) for x in operands[:2]]
        + [pltpu.SemaphoreType.DMA((3,))],
        compiler_params=PARAMS,
        cost_estimate=pl.CostEstimate(flops=1 << 34, bytes_accessed=1 << 20, transcendentals=0),
        name="table",
    )(*far(*operands))


def project_kernel(pairs, *refs):
    rows_refs, weights = refs[:pairs], refs[pairs:-2]
    keep_ref, send_ref = refs[-2:]
    _, seqs, _ = keep_ref.shape
    feats = weights[0].shape[0]
    rows = jnp.concatenate([ref[...].reshape(2 * seqs, feats) for ref in rows_refs], axis=0)
    start = 0
    for w in weights:
        cols = slice(start, start + w.shape[1])
        part = jnp.dot(rows, w[...], preferred_element_type=F32)
        for s in range(pairs):
            base = 2 * s * seqs
            keep_ref[s, :, cols] = part[base : base + seqs]
            send_ref[s, :, cols] = part[base + seqs : base + 2 * seqs].astype(BF16)
        start = cols.stop


def project(row_pairs, weights):
    chips = len(row_pairs)
    shape = (chips, row_pairs[0].shape[1], sum(w.shape[1] for w in weights))
    return call(
        lambda *refs: project_kernel(chips, *refs),
        (jax.ShapeDtypeStruct(shape, F32), jax.ShapeDtypeStruct(shape, BF16)),
    )(*row_pairs, *weights)


def chip_sum_kernel(keep_ref, crossed_ref, own_ref, *send_refs):
    own_ref[...] = keep_ref[0] + crossed_ref[0].astype(F32)
    for s, ref in enumerate(send_refs):
        ref[...] = (keep_ref[s + 1] + crossed_ref[s + 1].astype(F32)).astype(BF16)


def chip_sum(keep, crossed):
    chips, seqs, width = keep.shape
    sent = jax.ShapeDtypeStruct((seqs, width), BF16)
    out = (jax.ShapeDtypeStruct((seqs, width), F32),) + (sent,) * (chips - 1)
    own, *sends = call(chip_sum_kernel, out)(keep, crossed)
    return own, sends


def mix_kernel(heads_ref, *refs):
    *weights, out_ref = refs
    value = heads_ref[...]
    for j, w in enumerate(weights):
        width = w.shape[1]
        part = jnp.dot(value, w[...], preferred_element_type=F32)
        out_ref[:, j * width : (j + 1) * width] = part.astype(BF16)


def mix_heads(mixed_heads, weights):
    shape = (mixed_heads.shape[0], weights[0].shape[1] * len(weights))
    return call(mix_kernel, jax.ShapeDtypeStruct(shape, BF16))(mixed_heads, *weights)


def two_part(values, place, low):
    high = values.astype(BF16).astype(F32)
    return jnp.where(place < low, high, values - high).astype(BF16)


def middle_kernel(parts, tokens_ref, gains_ref, gate_ref, table_ref, *refs):
    pieces, (after_ref, packed_ref) = refs[:parts], refs[parts:]
    seqs, width = tokens_ref.shape
    ep_size = lax.axis_size("ep")
    feats = width // ep_size
    mine = lax.axis_index("ep")
    for j in range(ep_size):
        total = pieces[0][:, j * feats : (j + 1) * feats].astype(F32)
        for piece in pieces[1:]:
            total = total + piece[:, j * feats : (j + 1) * feats].astype(F32)
        cols = pl.ds(pl.multiple_of((mine ^ j) * feats, feats), feats)
        after_ref[:, cols] = total.astype(BF16).astype(F32)
    mix_wide = after_ref[...]
    after_mix = tokens_ref[...].astype(F32) + mix_wide * rms_scale(mix_wide) * gains_ref[1:2]
    after_ref[...] = after_mix
    ffn_in = (after_mix * rms_scale(after_mix) * gains_ref[2:3]).astype(BF16)
    packed_ref[:, :width] = ffn_in
    lanes = table_ref.shape[1]
    products = jnp.zeros((seqs, 128), F32)
    for j in range(width // 128):
        piece = packed_ref[:, j * 128 : (j + 1) * 128].astype(F32)
        products = products + piece * gate_ref[j : j + 1, :].astype(F32)
    dots = jnp.sum(products, axis=1, keepdims=True)
    place = lax.broadcasted_iota(jnp.int32, (seqs, lanes), 1)
    last = (place == ep_size) | (place == 2 * ep_size + 1)
    extra = jnp.where(last, jax.nn.sigmoid(dots), table_ref[...])
    packed_ref[:, width:] = two_part(extra, place, ep_size + 1)


def to_absolute(values, index, ep_size):
    rows, width = values.shape
    values = values.reshape(rows, ep_size, width // ep_size)
    order = index ^ jnp.arange(ep_size, dtype=jnp.int32)
    return jnp.take(values, order, axis=1).reshape(rows, width)


def plain_middle(tokens, norm_gains, dense_mix, table, pieces):
    ep_size = lax.axis_size("ep")
    total = total_of(pieces[0].astype(F32), pieces[1:])
    mix_wide = to_absolute(total.astype(BF16).astype(F32), lax.axis_index("ep"), ep_size)
    after_mix = tokens.astype(F32) + mix_wide * rms_scale(mix_wide) * norm_gains[1]
    ffn_in = (after_mix * rms_scale(after_mix) * norm_gains[2]).astype(BF16)
    dots = jnp.sum(ffn_in.astype(F32) * dense_mix.reshape(1, -1).astype(F32), axis=1, keepdims=True)
    place = jnp.arange(table.shape[1], dtype=jnp.int32)[None]
    last = (place == ep_size) | (place == 2 * ep_size + 1)
    extra = two_part(jnp.where(last, jax.nn.sigmoid(dots), table), place, ep_size + 1)
    return after_mix, jnp.concatenate([ffn_in, extra], axis=1)


def middle(tokens, norm_gains, dense_mix, table, pieces):
    seqs, width = tokens.shape
    lanes = table.shape[1]
    if (width // lax.axis_size("ep")) % 128:
        return plain_middle(tokens, norm_gains, dense_mix, table, pieces)
    return call(
        lambda *refs: middle_kernel(len(pieces), *refs),
        (
            jax.ShapeDtypeStruct((seqs, width), F32),
            jax.ShapeDtypeStruct((seqs, width + lanes), BF16),
        ),
    )(tokens, norm_gains, dense_mix, table, *near(pieces))


def dense_kernel(feats, even_ref, odd_ref, *refs):
    *weights, out_ref = refs
    half = out_ref.shape[1] // 2
    mine = lax.axis_index("ep")
    units = pl.ds(pl.multiple_of((mine & 1) * half, half), half)

    def features(index):
        cols = pl.ds(pl.multiple_of(index * feats, feats), feats)
        return jnp.concatenate([even_ref[:, cols], odd_ref[:, cols]], axis=0)

    own, other = features(mine), features(mine ^ 1)
    for k in range(2):
        part = jnp.dot(own, weights[k][:, units], preferred_element_type=F32) + jnp.dot(
            other, weights[2 + k][:, units], preferred_element_type=F32
        )
        out_ref[:, k * half : (k + 1) * half] = part.astype(out_ref.dtype)


def dense_part(even, odd, weights, dtype):
    feats, units = weights[0].shape
    half = units // 2
    if half % 128 or feats % 128:
        mine = lax.axis_index("ep")
        rows = jnp.concatenate([even, odd], axis=0)
        own, other = (
            lax.dynamic_slice_in_dim(rows, index * feats, feats, 1) for index in (mine, mine ^ 1)
        )
        picked = [lax.dynamic_slice_in_dim(w, (mine & 1) * half, half, 1) for w in weights]
        parts = [
            jnp.dot(own, picked[k], preferred_element_type=F32)
            + jnp.dot(other, picked[2 + k], preferred_element_type=F32)
            for k in range(2)
        ]
        return jnp.concatenate(parts, axis=1).astype(dtype)
    return call(
        lambda *refs: dense_kernel(feats, *refs),
        jax.ShapeDtypeStruct((2 * even.shape[0], units), dtype),
    )(even, odd, *weights)


def join_kernel(first, expert_ref, scale_ref, own_ref, other_ref, hidden_ref, keep_ref, send_ref):
    seqs = keep_ref.shape[0]
    half = own_ref.shape[0] // 2
    feats = own_ref.shape[1]
    mine = lax.axis_index("ep")
    units = pl.ds(pl.multiple_of((mine & 1) * half, half), half)
    rows = slice(first, first + seqs)
    others = slice(first + seqs, first + 2 * seqs)
    keep_ref[...] = expert_ref[rows]
    send_ref[...] = expert_ref[others].astype(BF16)
    scale = scale_ref[first : first + 2 * seqs]
    for weights, column in ((own_ref, mine), (other_ref, mine ^ 1)):
        dense = jnp.dot(hidden_ref[...], weights[units, :], preferred_element_type=F32) * scale
        cols = pl.ds(pl.multiple_of(column * feats, feats), feats)
        keep_ref[:, cols] += dense[:seqs]
        send_ref[:, cols] = (expert_ref[others, cols] + dense[seqs:]).astype(BF16)


def plain_join(rows, scale, down_own, down_other, hidden, seqs):
    ep_size = lax.axis_size("ep")
    mine = lax.axis_index("ep")
    count, width = rows.shape
    total = rows.reshape(count, ep_size, width // ep_size)
    column = jnp.arange(ep_size, dtype=jnp.int32)[None, :, None]
    for weights, place in ((down_own, mine), (down_other, mine ^ 1)):
        half = weights.shape[0] // 2
        picked = lax.dynamic_slice_in_dim(weights, (mine & 1) * half, half, 0)
        dense = jnp.dot(hidden, picked, preferred_element_type=F32) * scale
        total = total + jnp.where(column == place, dense[:, None, :], 0.0)
    total = total.reshape(count, width)
    return total[:seqs], total[seqs:].astype(BF16)


def join(expert_out, scale, down_own, down_other, hidden, chip, seqs):
    first = 2 * seqs * chip
    if down_own.shape[1] % 128:
        rows = slice(first, first + 2 * seqs)
        return plain_join(expert_out[rows], scale[rows], down_own, down_other, hidden, seqs)
    shape = (seqs, expert_out.shape[1])
    return call(
        lambda *refs: join_kernel(first, *refs),
        (jax.ShapeDtypeStruct(shape, F32), jax.ShapeDtypeStruct(shape, BF16)),
    )(expert_out, scale, down_own, down_other, hidden)


def core_sum_kernel(keep_ref, crossed_ref, out_ref):
    out_ref[...] = (keep_ref[...] + crossed_ref[...].astype(F32)).astype(out_ref.dtype)


def core_sum(keep, crossed, dtype):
    return call(core_sum_kernel, jax.ShapeDtypeStruct(keep.shape, dtype))(keep, crossed)


def finish_kernel(parts, after_ref, gains_ref, *refs):
    pieces, out_ref = refs[:parts], refs[parts]
    total = pieces[0][...].astype(F32)
    for piece in pieces[1:]:
        total = total + piece[...].astype(F32)
    scale = rms_scale(total)
    width = out_ref.shape[1]
    cols = pl.ds(pl.multiple_of(lax.axis_index("tp") * width, width), width)
    mine = pieces[0][:, cols].astype(F32)
    for piece in pieces[1:]:
        mine = mine + piece[:, cols].astype(F32)
    out_ref[...] = (after_ref[:, cols] + mine * scale * gains_ref[3:4, cols]).astype(BF16)


def finish(after_mix, norm_gains, pieces):
    seqs, width = after_mix.shape
    return call(
        lambda *refs: finish_kernel(len(pieces), *refs),
        jax.ShapeDtypeStruct((seqs, width // lax.axis_size("tp")), BF16),
    )(*near([after_mix, norm_gains, *pieces]))


def broadcast_column(columns, index, size):
    return jnp.broadcast_to(columns[:, index : index + 1], (size, size))


def read_kernel(arrived, *refs):
    own_ref, recv = refs[0], refs[1 : 1 + arrived]
    rows_ref, state_ref, mixed_ref, gates_ref = refs[1 + arrived :]
    seqs, heads, size, _ = state_ref.shape
    local = heads * size

    def column(kind, head):
        cols = slice(kind * local + head * size, kind * local + (head + 1) * size)
        value = own_ref[:, cols]
        for ref in recv:
            value = value + ref[:, cols].astype(F32)
        return value

    for head in range(heads):
        query_raw, forget_raw, value, out_gate = (column(kind, head) for kind in range(4))
        span = slice(head * size, (head + 1) * size)
        bound = rows_ref[0:1, span]
        forget = bound + (1.0 - bound) * jax.nn.sigmoid(forget_raw)
        key_in = (1.0 - bound) * jax.nn.sigmoid(-forget_raw)
        query = query_raw * jax.nn.sigmoid(query_raw)
        gates_ref[0, :, span] = forget
        gates_ref[1, :, span] = key_in
        gates_ref[2, :, span] = value
        weight = (query * forget).T
        rows = [
            jnp.sum(
                broadcast_column(weight, t, size) * state_ref[t, head], axis=0, keepdims=True
            )
            for t in range(seqs)
        ]
        read = jnp.concatenate(rows, axis=0)
        read = read + jnp.sum(query * key_in, axis=1, keepdims=True) * value
        gated = read * rms_scale(read) * rows_ref[1:2, span]
        mixed_ref[:, span] = (gated * (out_gate * jax.nn.sigmoid(out_gate))).astype(BF16)


def read_heads(own, arrived, head_rows, old_state):
    seqs, heads, size, _ = old_state.shape
    return call(
        lambda *refs: read_kernel(len(arrived), *refs),
        (
            jax.ShapeDtypeStruct((seqs, heads * size), BF16),
            jax.ShapeDtypeStruct((3, seqs, heads * size), F32),
        ),
    )(*near([own, *arrived, head_rows]), old_state)


def state_kernel(gates_ref, state_ref, *refs):
    out_ref = refs[-1]
    seqs, size = gates_ref.shape[1:]
    forget = gates_ref[0].T
    key_in = gates_ref[1].T
    for t in range(seqs):
        out_ref[t, 0] = (
            broadcast_column(forget, t, size) * state_ref[t, 0]
            + broadcast_column(key_in, t, size) * gates_ref[2, t : t + 1, :]
        )


def write_state(gates, old_state, first, count, partial=None):
    seqs, _, size, _ = old_state.shape
    block = pl.BlockSpec((seqs, 1, size, size), lambda h: (0, first + h, 0, 0))
    more = () if partial is None else (partial,)
    return pl.pallas_call(
        state_kernel,
        grid=(count,),
        in_specs=[pl.BlockSpec((3, seqs, size), lambda h: (0, 0, first + h)), block]
        + [pl.BlockSpec(memory_space=pl.ANY)] * len(more),
        out_specs=block,
        out_shape=jax.ShapeDtypeStruct(old_state.shape, F32),
        input_output_aliases={2: 0} if more else {},
        compiler_params=PARAMS,
        cost_estimate=pl.CostEstimate(
            flops=4 * old_state.size, bytes_accessed=8 * old_state.size, transcendentals=0
        ),
        name="write_state",
    )(gates, *(far(old_state) if partial is None else (old_state,)), *more)


def body(
    tokens,
    old_state,
    lower_bound,
    head_gain,
    norm_gains,
    w_query,
    w_forget,
    w_value,
    w_outgate,
    w_mix_out,
    routes,
    route_scores,
    w_exp_gate,
    w_exp_up,
    w_exp_down,
    w_dense_gate,
    w_dense_up,
    w_dense_down,
    dense_mix,
):
    seqs, width = tokens.shape
    ep_index = lax.axis_index("ep")
    ep_size = lax.axis_size("ep")

    mix_weights = background_gather(w_mix_out)

    dense_weights = (w_dense_gate, w_dense_up) + tuple(
        swap(w, "ep", 1) for w in (w_dense_gate, w_dense_up)
    )
    down_other = swap(w_dense_down, "ep", 1)
    low = ep_size + 1
    lanes = -(-2 * low // 128) * 128

    table, gate = route_table(routes, route_scores, dense_mix, lanes)
    even, odd, tokens, norm_gains, head_rows = front(
        tokens, norm_gains, lower_bound, head_gain, ep_size
    )
    row_pairs = relative_exchange(even, odd)
    keep, send = project(row_pairs, (w_query, w_forget, w_value, w_outgate))
    own, sends = chip_sum(keep, swap(send, "ep", 1))
    arrived = chip_send(sends)
    mixed_heads, gates = read_heads(own, arrived, head_rows, old_state)
    heads = old_state.shape[1]
    early = -(-heads // 2)
    new_state = write_state(gates, old_state, 0, early)
    if heads > early:
        new_state = write_state(gates, old_state, early, heads - early, new_state)
    mix_part = mix_heads(mixed_heads, mix_weights)
    mix_pieces = [mix_part] + tp_exchange(mix_part)
    after_mix, packed = middle(tokens, norm_gains, gate, table, mix_pieces)

    row_pairs = pair_gather(packed)
    dense_parts = []
    for s, (even, odd) in enumerate(row_pairs):
        dense_parts.append(dense_part(even, odd, dense_weights, BF16 if s else F32))
    dense_pre = total_of(dense_parts[0], chip_send(dense_parts[1:]))

    gathered = jnp.concatenate([item for pair in row_pairs for item in pair], axis=0)
    rows = gathered[:, :width]
    side = gathered[:, width:].astype(F32)
    side = side[:, :low] + side[:, low : 2 * low]
    expert_scale = lax.dynamic_slice_in_dim(side, ep_index, 1, 1)
    dense_scale = side[:, ep_size : ep_size + 1]

    dense_gate_pre, dense_up_pre = jnp.split(dense_pre, 2, axis=1)
    dense_hidden = (jax.nn.silu(dense_gate_pre) * dense_up_pre).astype(BF16)
    all_hidden = chip_gather(dense_hidden)

    gate_pre = jnp.dot(rows, w_exp_gate[0], preferred_element_type=F32)
    gate_pre = lax.optimization_barrier(gate_pre)
    up_pre = jnp.dot(rows, w_exp_up[0], preferred_element_type=F32)
    hidden = (jax.nn.silu(gate_pre) * up_pre).astype(BF16)
    hidden = lax.optimization_barrier(hidden)
    expert_out = jnp.dot(hidden, w_exp_down[0], preferred_element_type=F32) * expert_scale
    expert_out = lax.optimization_barrier(expert_out)
    sums = []
    for chip, hidden_rows in enumerate(all_hidden):
        keep, send = join(
            expert_out, dense_scale, w_dense_down, down_other, hidden_rows, chip, seqs
        )
        sums.append(core_sum(keep, swap(send, "ep", 1), BF16 if chip else F32))
    ffn_part = total_of(sums[0], chip_send(sums[1:])).astype(BF16)
    ffn_pieces = [ffn_part] + tp_exchange(ffn_part)
    return (finish(after_mix, norm_gains, ffn_pieces), new_state)


def solution(mesh):
    return jax.shard_map(
        body,        mesh=mesh,
        in_specs=(
            P("ep", None),
            P("ep", "tp", None, None),
            P("tp"),
            P("tp"),
            P(),
            P("ep", "tp"),
            P("ep", "tp"),
            P("ep", "tp"),
            P("ep", "tp"),
            P("tp", "ep"),
            P("ep", None),
            P("ep", None),
            P("ep", None, "tp"),
            P("ep", None, "tp"),
            P("ep", "tp", None),
            P("ep", "tp"),
            P("ep", "tp"),
            P("tp", "ep"),
            P(),
        ),
        out_specs=(P("ep", "tp"), P("ep", "tp", None, None)),
        check_vma=False,
    )
```
